32 devices in a mesh: dp: 4 (over y, x), kv: 4 (over z), tp: 2 (over core).
Axes of the slice: x: 2, y: 2, z: 4, core: 2. Of those that a mesh axis runs over, the one named last changes fastest.
Arguments:
- tokens: bfloat16 [32, 4, 2048], P('dp', None, 'kv'), may hold values from -600 to 600
- input_norm_gain: float32 [2048], P('kv'), may hold values from 0.1 to 1.9
- query_projection: bfloat16 [2048, 1024], P('kv', 'tp'), may hold values from -0.125 to 0.125
- key_projection: bfloat16 [2048, 1024], P('kv', 'tp'), may hold values from -0.125 to 0.125
- value_projection: bfloat16 [2048, 1024], P('kv', 'tp'), may hold values from -0.125 to 0.125
- write_strength_weight: bfloat16 [2048, 16], P('kv', 'tp'), may hold values from -0.125 to 0.125
- decay_projection: bfloat16 [2048, 16], P('kv', 'tp'), may hold values from -0.125 to 0.125
- head_decay_rate: float32 [16], P('tp'), may hold values from 0.02 to 0.6
- token_extra_decay: float32 [32, 4, 16], P(('dp', 'kv'), None, 'tp'), may hold values from -0.7 to 0
- accepted: int32 [32], P(('dp', 'kv')), may hold values from 1 to 4
- prior_step_states: float32 [32, 4, 16, 4096], P(('dp', 'kv'), None, 'tp'), may hold values from -4 to 4
- output_norm_gain: float32 [64], replicated, may hold values from 0.1 to 1.9
- output_projection: bfloat16 [1024, 2048], P('tp', 'kv'), may hold values from -0.1875 to 0.1875
Outputs:
- mixed: bfloat16 [32, 4, 2048], P('dp', None, 'kv')
- updated_states: float32 [32, 4, 16, 4096], P(('dp', 'kv'), None, 'tp')
The draws below stay inside these ranges and needn't reach their ends.
Inputs may be any that keep to these rules, and one draw needn't show every extreme that they name: `accepted`: how many proposals of the previous step each sequence kept; its state after that many is taken up.
All inputs are finite; a program needn't handle non-finite values.
Results may differ from the reference program's by a relative error of at most 0.029.
Values may be sent and summed in bfloat16 or wider, within the bound.
A program may use at most 64 MiB of HBM per device.

```python
import math
import jax
import jax.numpy as jnp
from jax import lax

D = 2048
HEAD_TOTAL = 16
HEAD = 64
DRAFT_TOKENS = 4
SEQ_DEV = 2
SEQUENCE_TOTAL = 32


def draw_tokens(key, part):
    base_key = jax.random.fold_in(key, 11)
    key_one = jax.random.fold_in(base_key, 0)
    column = jnp.arange(D, dtype=jnp.float32) / D
    sample_noise = jax.random.normal(key_one, (SEQUENCE_TOTAL, DRAFT_TOKENS, D), jnp.float32)
    values = sample_noise * 10.0 ** column
    return values.astype(jnp.bfloat16)


def place_ends(array, own_key, least, largest):
    place = [jax.random.randint(jax.random.fold_in(own_key, axis), (), 0, length) for axis, length in enumerate(array.shape)]
    longest = array.shape.index(max(array.shape))
    next_to = place[:longest] + [(place[longest] + 1) % array.shape[longest]] + place[longest + 1:]
    return array.at[tuple(place)].set(least).at[tuple(next_to)].set(largest)


def shard_levels(key, extent, pieces, smallest, largest):
    factor_of, own = 1.0, jax.random.fold_in(key, 6)
    for dim, parts in pieces:
        heights = jnp.exp(jax.random.uniform(jax.random.fold_in(own, dim), (parts,), jnp.float32, smallest / len(pieces), largest / len(pieces)))
        factor_of = factor_of * jnp.repeat(heights, extent[dim] // parts).reshape([-1 if axis == dim else 1 for axis in range(len(extent))])
    return factor_of


def scatter_about(own_key, extent, scale, bound, cuts=(), held_as=jnp.bfloat16):
    array = jax.random.normal(own_key, extent, jnp.float32) * scale
    if len(cuts) > 0:
        array = shard_levels(own_key, extent, cuts, -0.22, 0.18) * array
    return jnp.clip(array, min=-bound, max=bound).astype(held_as)


def setup_inputs(seed: int = 0) -> dict:
    key_list = jax.random.split(jax.random.key(seed), 14)
    tokens = draw_tokens(jax.random.fold_in(key_list[13], 71), 0)
    input_norm_gain = jnp.clip(1.0 + 0.18 * jax.random.normal(key_list[1], (D,), jnp.float32), 0.1, 1.9)
    query_projection = scatter_about(key_list[2], (D, HEAD_TOTAL * HEAD), D ** -0.5, 0.125, ((0, 4), (1, 2)))
    key_projection = scatter_about(key_list[3], (D, HEAD_TOTAL * HEAD), D ** -0.5, 0.125, ((0, 4), (1, 2)))
    value_projection = scatter_about(key_list[4], (D, HEAD_TOTAL * HEAD), D ** -0.5, 0.125, ((0, 4), (1, 2)))
    write_strength_weight = scatter_about(key_list[5], (D, HEAD_TOTAL), D ** -0.5, 0.125, ((0, 4), (1, 2)))
    decay_projection = scatter_about(key_list[6], (D, HEAD_TOTAL), D ** -0.5, 0.125, ((0, 4), (1, 2)))
    head_decay_rate = jnp.clip(jnp.exp(math.log(0.6) - 3.4011974 * jax.random.uniform(key_list[7], (HEAD_TOTAL,), jnp.float32) ** shard_levels(key_list[7], (HEAD_TOTAL,), ((0, 2),), -0.2, 0.2)), 0.02, 0.6)
    token_extra_decay = jnp.clip(-0.7 + 0.7 * jax.random.uniform(key_list[8], (SEQUENCE_TOTAL, DRAFT_TOKENS, HEAD_TOTAL), jnp.float32) ** shard_levels(key_list[8], (SEQUENCE_TOTAL, DRAFT_TOKENS, HEAD_TOTAL), ((0, 16), (2, 2)), -0.2, 0.2), -0.7, 0.0)
    accepted = place_ends(jax.random.randint(key_list[9], (SEQUENCE_TOTAL,), 1, DRAFT_TOKENS + 1), jax.random.fold_in(key_list[9], 1), 1, DRAFT_TOKENS).astype(jnp.int32)
    prior_step_states = scatter_about(key_list[10], (SEQUENCE_TOTAL, DRAFT_TOKENS, HEAD_TOTAL, HEAD * HEAD), 0.3, 4.0, ((0, 16), (2, 2)), jnp.float32)
    output_norm_gain = jnp.clip(1.0 + 0.18 * jax.random.normal(key_list[11], (HEAD,), jnp.float32), 0.1, 1.9)
    output_projection = scatter_about(key_list[12], (HEAD_TOTAL * HEAD, D), (HEAD_TOTAL * HEAD) ** -0.5, 0.1875, ((0, 2), (1, 4)))
    return {"tokens": tokens, "input_norm_gain": input_norm_gain, "query_projection": query_projection, "key_projection": key_projection, "value_projection": value_projection, "write_strength_weight": write_strength_weight, "decay_projection": decay_projection, "head_decay_rate": head_decay_rate, "token_extra_decay": token_extra_decay, "accepted": accepted, "prior_step_states": prior_step_states, "output_norm_gain": output_norm_gain, "output_projection": output_projection}


epsilon = 1e-06
highest = lax.Precision.HIGHEST

def unit_rows(values):
    return values * lax.rsqrt(lax.optimization_barrier(jnp.sum(values * values, axis=-1, keepdims=True)) + epsilon)

def delta_block(query_heads, key_heads, value_heads, beta_gate, decay_logarithm, start_state):
    proposal_len = query_heads.shape[2]
    cumulative = jnp.cumsum(decay_logarithm, axis=-1)
    spread = cumulative[..., :, None] - cumulative[..., None, :]
    strict = jnp.tril(jnp.ones((proposal_len, proposal_len), bool), -1)
    inclusive = jnp.tril(jnp.ones((proposal_len, proposal_len), bool))
    key_inner = jnp.einsum('nhid,nhjd->nhij', key_heads, key_heads, precision=highest)
    coupling = jnp.where(strict, beta_gate[..., :, None] * key_inner * jnp.exp(jnp.where(strict, spread, 0.0)), 0.0)
    growth = jnp.exp(cumulative)
    right_w = (beta_gate * growth)[..., None] * key_heads
    right_u = beta_gate[..., None] * value_heads
    solved_w = []
    solved_u = []
    for current in range(proposal_len):
        part_w = right_w[:, :, current]
        part_u = right_u[:, :, current]
        for earlier in range(current):
            factor = coupling[:, :, current, earlier][..., None]
            part_w = part_w - factor * solved_w[earlier]
            part_u = part_u - factor * solved_u[earlier]
        solved_w.append(part_w)
        solved_u.append(part_u)
    weights_w = jnp.stack(solved_w, axis=2)
    weights_u = jnp.stack(solved_u, axis=2)
    corrected = weights_u - jnp.einsum('nhpd,nhde->nhpe', weights_w, start_state, precision=highest)
    within = jnp.where(inclusive, jnp.exp(jnp.where(inclusive, spread, 0.0)), 0.0)
    scores = jnp.einsum('nhid,nhjd->nhij', query_heads, key_heads, precision=highest) * within
    attended = jnp.einsum('nhpd,nhde->nhpe', query_heads * growth[..., None], start_state, precision=highest) + jnp.einsum('nhij,nhje->nhie', scores, corrected, precision=highest)
    states = growth[..., None, None] * start_state[:, :, None] + jnp.einsum('nhtj,nhjd,nhje->nhtde', within, key_heads, corrected, precision=highest)
    return (attended, states)

def combine_heads(query_logits, key_logits, value_logits, beta_logits, decay_logits, head_decay_rate, token_extra_decay, accepted, prior_step_states, output_norm_gain):
    seq_count, proposal_len, head_count = beta_logits.shape
    head_size = query_logits.shape[-1] // head_count

    def by_heads(values):
        return jnp.transpose(values.reshape(seq_count, proposal_len, head_count, head_size), (0, 2, 1, 3))
    query_heads = unit_rows(by_heads(jax.nn.silu(query_logits))) * head_size ** (-0.5)
    key_heads = unit_rows(by_heads(jax.nn.silu(key_logits)))
    value_heads = by_heads(jax.nn.silu(value_logits))
    beta_gate = jnp.transpose(jax.nn.sigmoid(beta_logits), (0, 2, 1))
    decay_logarithm = jnp.transpose(-head_decay_rate[None, None, :] * jax.nn.softplus(decay_logits) + token_extra_decay, (0, 2, 1))
    chosen = jnp.arange(proposal_len, dtype=jnp.int32)[None, :] == (accepted - 1)[:, None]
    picked = lax.optimization_barrier(jnp.sum(jnp.where(chosen[:, :, None, None], prior_step_states, 0.0), axis=1))
    start_state = picked.reshape(seq_count, head_count, head_size, head_size)
    attended, states = delta_block(query_heads, key_heads, value_heads, beta_gate, decay_logarithm, start_state)
    inverse_rms = lax.rsqrt(lax.optimization_barrier(jnp.mean(attended * attended, axis=-1, keepdims=True)) + epsilon)
    normalized_rows = (attended * inverse_rms * output_norm_gain).astype(jnp.bfloat16)
    normalized_rows = jnp.transpose(normalized_rows, (0, 2, 1, 3)).reshape(seq_count, proposal_len, head_count * head_size)
    updated_states = jnp.transpose(states, (0, 2, 1, 3, 4)).reshape(seq_count, proposal_len, head_count, head_size * head_size)
    return (normalized_rows, updated_states)

def reference(tokens, input_norm_gain, query_projection, key_projection, value_projection, write_strength_weight, decay_projection, head_decay_rate, token_extra_decay, accepted, prior_step_states, output_norm_gain, output_projection):
    seq_total, proposal_len, feature_count = tokens.shape
    token_rows = tokens.reshape(seq_total * proposal_len, feature_count).astype(jnp.float32)
    inverse = lax.rsqrt(lax.optimization_barrier(jnp.sum(token_rows * token_rows, axis=1)) / feature_count + epsilon)[:, None]
    scaled = (token_rows * input_norm_gain[None, :]).astype(jnp.bfloat16)

    def apply_projection(weight):
        result = jnp.dot(scaled, weight, preferred_element_type=jnp.float32) * inverse
        return result.reshape(seq_total, proposal_len, weight.shape[1])
    block_count = seq_total // SEQ_DEV

    def divide_blocks(values):
        return values.reshape((block_count, SEQ_DEV) + values.shape[1:])

    def single_block(input_rows):
        query_logits, key_logits, value_logits, beta_logits, decay_logits, extra_decay_slice, accepted_slice, saved_slice = input_rows
        return combine_heads(query_logits, key_logits, value_logits, beta_logits, decay_logits, head_decay_rate, extra_decay_slice, accepted_slice, saved_slice, output_norm_gain)
    normalized_rows, updated_states = lax.map(single_block, (divide_blocks(apply_projection(query_projection)), divide_blocks(apply_projection(key_projection)), divide_blocks(apply_projection(value_projection)), divide_blocks(apply_projection(write_strength_weight)), divide_blocks(apply_projection(decay_projection)), divide_blocks(token_extra_decay), divide_blocks(accepted), divide_blocks(prior_step_states)))
    normed_rows = normalized_rows.reshape(seq_total * proposal_len, output_projection.shape[0])
    mixed = jnp.dot(normed_rows, output_projection, preferred_element_type=jnp.float32).astype(jnp.bfloat16)
    return (mixed.reshape(seq_total, proposal_len, feature_count), updated_states.reshape(prior_step_states.shape))
```

```python
import functools
import jax
import jax.numpy as jnp
from jax import lax
from jax.experimental import pallas as pl
from jax.experimental.pallas import tpu as pltpu
from jax.sharding import PartitionSpec as P

epsilon = 1e-06
MESH = pl.DeviceIdType.MESH
f32 = jnp.float32
bf16 = jnp.bfloat16
LANES = 128
VMEM_LIMIT = 32 * 2 ** 20


def silu(u):
    return u / (1.0 + jnp.exp(-u))


def wait_bytes(ref, sem):
    pltpu.make_async_copy(ref, ref, sem).wait()


def kernel(
    n,
    ntp,
    head_size,
    tokens_hbm,
    gain_hbm,
    wq_hbm,
    wk_hbm,
    wv_hbm,
    wb_hbm,
    wd_hbm,
    rate_hbm,
    extra_hbm,
    accepted_hbm,
    prior_hbm,
    onorm_hbm,
    wo_hbm,
    mixed_ref,
    states_v,
    tokens_v,
    gain_v,
    w_v,
    wbd_v,
    rate_v,
    extra_v,
    accepted_s,
    prior_v,
    onorm_v,
    wo_v,
    x_v,
    aux_v,
    send_v,
    recv_v,
    start_v,
    block_v,
    limits_v,
    spread_v,
    ones_v,
    tall_v,
    normed_v,
    recvn_v,
    parts_v,
    heads_v,
    expand_v,
    load_sem,
    regular_sem,
    send_sem,
    recv_sem,
):
    me = lax.axis_index("kv")
    my_tp = lax.axis_index("tp")
    root = ntp - 1
    is_root = my_tp == root
    group_seqs, steps, feature_dev = tokens_v.shape
    own_seqs, _, heads, state_len = prior_v.shape
    own_rows = own_seqs * steps
    model_width = n * feature_dev
    inner = heads * head_size
    pairs = inner // LANES
    blocks = ntp * pairs
    per_block = LANES // head_size
    RS, START, LIMITS, WO, GATHER, PARTS, GATHER_ROOT = range(7)
    here = regular_sem.at[0]

    def device(o, p):
        return {"kv": lax.rem(me + o, n), "tp": p}

    barrier = pltpu.get_barrier_semaphore()

    @pl.when(is_root)
    def _():
        for o in range(1, n):
            pl.semaphore_signal(
                barrier, inc=1, device_id=device(o, root), device_id_type=MESH
            )
        for p in range(root):
            for o in range(n):
                pl.semaphore_signal(
                    barrier, inc=1, device_id=device(o, p), device_id_type=MESH
                )

    loads = {}
    for index, (name, source, target) in enumerate((
        ("tokens", tokens_hbm, tokens_v),
        ("gain", gain_hbm, gain_v),
        ("wb", wb_hbm, wbd_v.at[0]),
        ("wd", wd_hbm, wbd_v.at[1]),
        ("q", wq_hbm, w_v.at[0]),
        ("k", wk_hbm, w_v.at[1]),
        ("v", wv_hbm, w_v.at[2]),
        ("prior", prior_hbm, prior_v),
        ("rate", rate_hbm, rate_v),
        ("extra", extra_hbm, extra_v),
        ("accepted", accepted_hbm, accepted_s),
        ("onorm", onorm_hbm, onorm_v),
        ("wo", wo_hbm, wo_v.at[my_tp]),
    )):
        loads[name] = pltpu.make_async_copy(source, target, load_sem.at[index])
        loads[name].start()

    loads["tokens"].wait()
    loads["gain"].wait()
    for s in range(group_seqs):
        x_v[s * steps:(s + 1) * steps, :] = tokens_v[s].astype(f32)
    x = x_v[...]
    squares = jnp.sum(x * x, axis=1, keepdims=True)
    scaled = (x * gain_v[...]).astype(bf16)

    contract_last = (((1,), (1,)), ((), ()))
    loads["wb"].wait()
    loads["wd"].wait()
    lane_x = lax.broadcasted_iota(jnp.int32, (x.shape[0], LANES), 1)
    half = LANES // 2
    aux_v[...] = jnp.where(lane_x >= half, squares, 0.0)
    for index in range(2):
        aux_v[:, index * heads:(index + 1) * heads] = lax.dot_general(
            scaled, wbd_v[index], contract_last, preferred_element_type=f32
        )
    send_v[:, :, 3 * inner:3 * inner + LANES] = (
        aux_v[...].reshape(n, own_rows, LANES).astype(bf16)
    )
    send_v[:, :, 3 * inner + LANES:] = (
        jnp.where(lane_x < half, squares, 0.0).reshape(n, own_rows, LANES).astype(bf16)
    )
    for piece, name in enumerate("qkv"):
        loads[name].wait()
        part = jnp.dot(scaled, w_v[piece], preferred_element_type=f32)
        send_v[:, :, piece * inner:(piece + 1) * inner] = (
            part.reshape(n, own_rows, inner).astype(bf16)
        )

    def remote(source, target, kind, where):
        pltpu.make_async_remote_copy(
            src_ref=source,
            dst_ref=target,
            send_sem=send_sem.at[kind],
            recv_sem=recv_sem.at[GATHER if kind == GATHER_ROOT else kind],
            device_id=where,
            device_id_type=MESH,
        ).start()

    @pl.when(is_root)
    def _():
        pl.semaphore_wait(barrier, n - 1)
        for o in range(1, n):
            remote(send_v.at[lax.rem(me + o, n)], recv_v.at[o - 1], RS, device(o, root))

    @pl.when(jnp.logical_not(is_root))
    def _():
        pl.semaphore_wait(barrier, n)
        for o in range(n):
            remote(
                send_v.at[lax.rem(me + o, n)], recv_v.at[n - 1 + my_tp * n + o], RS,
                device(o, root),
            )
        for o in range(n):
            pl.semaphore_signal(here, inc=1, device_id=device(o, root), device_id_type=MESH)

    for name in ("rate", "extra", "accepted", "onorm", "prior"):
        loads[name].wait()

    limits_v[my_tp] = jnp.zeros(limits_v.shape[1:], f32)
    limits_v[my_tp, 0, :, heads:2 * heads] = jnp.broadcast_to(rate_v[...], (own_rows, heads))
    for s in range(own_seqs):
        limits_v[my_tp, 1, s * steps:(s + 1) * steps, heads:2 * heads] = extra_v[s]

    lane = lax.broadcasted_iota(jnp.int32, (heads, LANES), 1)
    head = lax.broadcasted_iota(jnp.int32, (heads, LANES), 0)
    first_half = lane < head_size
    even_head = lax.rem(head, 2) == 0
    diagonal = first_half == even_head
    for s in range(own_seqs):
        state = prior_v[s, jnp.clip(accepted_s[s] - 1, 0, steps - 1)]
        for j in range(state_len // LANES):
            both = state[:, j * LANES:(j + 1) * LANES]
            turned = pltpu.roll(both, head_size, 1)
            for half_index, right_lanes in ((0, even_head), (1, jnp.logical_not(even_head))):
                rows = jnp.where(diagonal, jnp.where(right_lanes, both, turned), 0.0)
                start_v[s, pl.ds(2 * j + half_index, heads, stride=head_size), :] = rows
        block_v[my_tp, :, s * LANES:(s + 1) * LANES] = start_v[s].astype(bf16)

    @pl.when(jnp.logical_not(is_root))
    def _():
        remote(block_v.at[my_tp], block_v.at[my_tp], START, device(0, root))
        remote(limits_v.at[my_tp], limits_v.at[my_tp], LIMITS, device(0, root))

    loads["wo"].wait()

    @pl.when(jnp.logical_not(is_root))
    def _():
        remote(wo_v.at[my_tp], wo_v.at[my_tp], WO, device(0, root))

    @pl.when(is_root)
    def _():
        pl.semaphore_wait(here, n * root)
        for p in range(root):
            remote(wo_v.at[my_tp], wo_v.at[my_tp], WO, device(0, p))

    entry = lax.broadcasted_iota(jnp.int32, spread_v.shape, 0)
    column = lax.broadcasted_iota(jnp.int32, spread_v.shape, 1)
    first = jnp.where(entry < head_size, entry, entry - head_size) * head_size
    spread_v[...] = jnp.where(
        (column >= first) & (column < first + head_size), 1.0, 0.0
    ).astype(bf16)
    entry = lax.broadcasted_iota(jnp.int32, ones_v.shape, 0)
    column = lax.broadcasted_iota(jnp.int32, ones_v.shape, 1)
    ones_v[...] = jnp.where(
        (entry < head_size) == (column < head_size), 1.0, 0.0
    ).astype(bf16)

    Q, K, V, QS, KS, BETA, DECAY = range(7)

    def tall(item, s, t):
        row = (s * steps + t) * blocks
        return tall_v[item, row:row + blocks, :]

    def heads_of(p):
        for item in range(3):
            for pair in range(pairs):
                value = parts_v[item, pl.ds(p * pairs + pair, own_rows, stride=blocks), :]
                turned = pltpu.roll(value, head_size, 1)
                left = lax.broadcasted_iota(jnp.int32, value.shape, 1) < head_size
                for sub, (one, two) in enumerate(((value, turned), (turned, value))):
                    heads_v[item, pl.ds(pair * per_block + sub, own_rows, stride=heads), :] = (
                        jnp.where(left, one, two)
                    )

    @pl.when(is_root)
    def _():
        row_lane = lax.broadcasted_iota(jnp.int32, (own_rows, LANES), 1)
        row_first = row_lane < head_size
        row_seq = lax.broadcasted_iota(jnp.int32, (2 * own_rows, LANES), 0)
        row_seq = lax.rem(row_seq, own_rows)
        wait_bytes(recv_v, recv_sem.at[RS])
        for p in range(root):
            wait_bytes(block_v.at[p], recv_sem.at[START])
            wait_bytes(limits_v.at[p], recv_sem.at[LIMITS])
        for p in range(ntp):
            if p == root:
                parts = [send_v[me].astype(f32)]
                parts += [recv_v[o - 1].astype(f32) for o in range(1, n)]
            else:
                parts = [recv_v[n - 1 + p * n + o].astype(f32) for o in range(n)]
            total = functools.reduce(jnp.add, parts)
            low_block = total[:, 3 * inner:3 * inner + LANES]
            high_block = total[:, 3 * inner + LANES:]
            inverse = lax.rsqrt(
                jnp.where(row_lane < half, high_block, low_block) / model_width + epsilon
            )
            gates = low_block * inverse
            beta = 1.0 / (1.0 + jnp.exp(-gates))
            softplus = jnp.maximum(gates, 0.0) + jnp.log1p(jnp.exp(-jnp.abs(gates)))
            decay = jnp.exp(limits_v[p, 1] - limits_v[p, 0] * softplus)
            for pair in range(pairs):
                block = p * pairs + pair
                rows = pl.ds(block, own_rows, stride=blocks)
                values = [
                    silu(
                        total[:, c * inner + pair * LANES:c * inner + (pair + 1) * LANES]
                        * inverse
                    )
                    for c in range(3)
                ]
                for item in (Q, K, V):
                    tall_v[item, rows, :] = values[item]
                both = jnp.concatenate([values[Q], values[K]], axis=0).astype(bf16)
                product = jnp.dot(
                    both, block_v[p, pair * LANES:(pair + 1) * LANES, :],
                    preferred_element_type=f32,
                )
                chosen = product[:, 0:LANES]
                for s in range(1, own_seqs):
                    chosen = jnp.where(
                        row_seq >= s * steps, product[:, s * LANES:(s + 1) * LANES], chosen
                    )
                tall_v[QS, rows, :] = chosen[:own_rows]
                tall_v[KS, rows, :] = chosen[own_rows:]
                for item, gate, offset in ((BETA, beta, 0), (DECAY, decay, heads)):
                    place = offset + pair * per_block
                    tall_v[item, rows, :] = jnp.where(
                        row_first, gate[:, place:place + 1], gate[:, place + 1:place + 2]
                    )

        products = []
        for s in range(own_seqs):
            for t in range(steps):
                query, key = tall(Q, s, t), tall(K, s, t)
                products += [query * query, key * key]
                for j in range(t):
                    products += [key * tall(K, s, j), query * tall(K, s, j)]
                products.append(query * key)
        products = jnp.concatenate(products, axis=0).astype(bf16)
        sums = jnp.dot(products, ones_v[...], preferred_element_type=f32)
        sums = iter([sums[i * blocks:(i + 1) * blocks] for i in range(sums.shape[0] // blocks)])
        attended = []
        writes = []
        keys = []
        for s in range(own_seqs):
            query_scale, key_scale, key_dots, query_dots = [], [], {}, {}
            for t in range(steps):
                query_scale.append(lax.rsqrt(next(sums) + epsilon) * head_size ** -0.5)
                key_scale.append(lax.rsqrt(next(sums) + epsilon))
                for j in range(t):
                    key_dots[t, j] = next(sums) * (key_scale[t] * key_scale[j])
                    query_dots[t, j] = next(sums) * (query_scale[t] * key_scale[j])
                query_dots[t, t] = next(sums) * (query_scale[t] * key_scale[t])
            write = []
            grown = None
            spans = []
            for t in range(steps):
                decay, beta = tall(DECAY, s, t), tall(BETA, s, t)
                grown = decay if t == 0 else grown * decay
                spans = [span * decay for span in spans]
                held = grown * key_scale[t] * tall(KS, s, t)
                seen = grown * query_scale[t] * tall(QS, s, t)
                for j in range(t):
                    held = held + spans[j] * key_dots[t, j] * write[j]
                    seen = seen + spans[j] * query_dots[t, j] * write[j]
                write.append(beta * (tall(V, s, t) - held))
                spans.append(jnp.ones_like(decay))
                attended.append(seen + query_dots[t, t] * write[t])
            writes += write
            keys += key_scale
        squared = jnp.concatenate([a * a for a in attended], axis=0).astype(bf16)
        means = jnp.dot(squared, ones_v[...], preferred_element_type=f32) / head_size
        norm_gain = jnp.concatenate([onorm_v[...]] * per_block, axis=1)
        for row in range(own_rows):
            scale = lax.rsqrt(means[row * blocks:(row + 1) * blocks] + epsilon)
            normed_v[row * blocks:(row + 1) * blocks, :] = attended[row] * scale * norm_gain
        for block in range(blocks):
            recvn_v[me, :, block * LANES:(block + 1) * LANES] = (
                normed_v[pl.ds(block, own_rows, stride=blocks), :].astype(bf16)
            )
        for o in range(1, n):
            remote(recvn_v.at[me], recvn_v.at[me], GATHER_ROOT, device(o, root))
        for p in range(root):
            for o in range(n):
                remote(recvn_v.at[me], recvn_v.at[me], GATHER, device(o, p))
        for s in range(own_seqs):
            for t in range(steps):
                row = s * steps + t
                rows = slice(row * blocks, (row + 1) * blocks)
                parts_v[0, rows, :] = tall(K, s, t) * keys[row]
                parts_v[1, rows, :] = writes[row]
                parts_v[2, rows, :] = tall(DECAY, s, t)
        for p in range(root):
            remote(parts_v, parts_v, PARTS, device(0, p))
        heads_of(root)

    @pl.when(jnp.logical_not(is_root))
    def _():
        wait_bytes(parts_v, recv_sem.at[PARTS])
        for p in range(root):
            @pl.when(my_tp == p)
            def _():
                heads_of(p)

    keys = heads_v[0, :, 0:head_size]
    high = keys.astype(bf16)
    low = (keys - high.astype(f32)).astype(bf16)
    both = jnp.concatenate([high.astype(f32), low.astype(f32)], axis=1).astype(bf16)
    expand_v[...] = jnp.dot(both, spread_v[...], preferred_element_type=f32)

    def wide(value):
        return jnp.concatenate([value] * (state_len // LANES), axis=1)

    for s in range(own_seqs):
        state = prior_v[s, jnp.clip(accepted_s[s] - 1, 0, steps - 1)]
        for t in range(steps):
            block = slice((s * steps + t) * heads, (s * steps + t + 1) * heads)
            state = wide(heads_v[2, block, :]) * state + (
                expand_v[block, :] * wide(heads_v[1, block, :])
            )
            states_v[s, t] = state

    for p in range(root):
        wait_bytes(wo_v.at[p], recv_sem.at[WO])

    @pl.when(is_root)
    def _():
        wait_bytes(recvn_v.at[pl.ds(0, n - 1)], recv_sem.at[GATHER])

    @pl.when(jnp.logical_not(is_root))
    def _():
        wait_bytes(recvn_v, recv_sem.at[GATHER])

    rows = recvn_v[...].reshape(n * own_rows, ntp * inner)
    weights = wo_v[...].reshape(ntp * inner, wo_v.shape[2])
    mixed = jnp.dot(rows, weights, preferred_element_type=f32)
    for s in range(group_seqs):
        mixed_ref[s] = mixed[s * steps:(s + 1) * steps].astype(bf16)

    for p in range(root):
        wait_bytes(wo_v.at[p], send_sem.at[WO])

    @pl.when(is_root)
    def _():
        wait_bytes(send_v.at[pl.ds(0, n - 1)], send_sem.at[RS])
        wait_bytes(recvn_v.at[pl.ds(0, n - 1)], send_sem.at[GATHER_ROOT])
        for p in range(root):
            wait_bytes(recvn_v, send_sem.at[GATHER])
            wait_bytes(parts_v, send_sem.at[PARTS])

    @pl.when(jnp.logical_not(is_root))
    def _():
        wait_bytes(send_v, send_sem.at[RS])
        wait_bytes(block_v.at[0], send_sem.at[START])
        wait_bytes(limits_v.at[0], send_sem.at[LIMITS])


def finish(mixed_v, states_v, mixed_hbm, states_hbm, sem):
    own_seqs, steps = states_v.shape[:2]
    copies = [
        pltpu.make_async_copy(
            states_v.at[s, t], states_hbm.at[s, t], sem.at[1 + s * steps + t]
        )
        for s in range(own_seqs)
        for t in range(steps)
    ]
    copies.append(pltpu.make_async_copy(mixed_v, mixed_hbm, sem.at[0]))
    for copy in copies:
        copy.start()
    for copy in copies:
        copy.wait()


def per_device(n, ntp, *args):
    (
        tokens, input_norm_gain, query_projection, key_projection, value_projection,
        write_strength_weight, decay_projection, head_decay_rate, token_extra_decay,
        accepted, prior_step_states, output_norm_gain, output_projection,
    ) = args
    group_seqs, steps, feature_dev = tokens.shape
    own_seqs, _, heads, state_len = prior_step_states.shape
    own_rows = own_seqs * steps
    head_size = output_norm_gain.shape[0]
    inner = query_projection.shape[1]
    out_dev = output_projection.shape[1]
    rows = group_seqs * steps
    pairs = inner // LANES
    blocks = ntp * pairs
    width = 3 * inner + 2 * LANES
    any_spec = pl.BlockSpec(memory_space=pl.ANY)
    vmem_spec = pl.BlockSpec(memory_space=pltpu.VMEM)
    dma = pltpu.SemaphoreType.DMA

    def hbm(array):
        return pltpu.with_memory_space_constraint(array, pltpu.HBM)

    mixed, states = pl.pallas_call(
        functools.partial(kernel, n, ntp, head_size),
        out_shape=(
            pltpu.VMEM((group_seqs, steps, out_dev), bf16),
            pltpu.VMEM(prior_step_states.shape, f32),
        ),
        in_specs=[any_spec] * 13,
        out_specs=(vmem_spec, vmem_spec),
        scratch_shapes=[
            pltpu.VMEM(tokens.shape, bf16),
            pltpu.VMEM((1, feature_dev), f32),
            pltpu.VMEM((3, feature_dev, inner), bf16),
            pltpu.VMEM((2, heads, feature_dev), bf16),
            pltpu.VMEM((1, heads), f32),
            pltpu.VMEM(token_extra_decay.shape, f32),
            pltpu.SMEM(accepted.shape, jnp.int32),
            pltpu.VMEM(prior_step_states.shape, f32),
            pltpu.VMEM((1, head_size), f32),
            pltpu.VMEM((ntp, inner, out_dev), bf16),
            pltpu.VMEM((rows, feature_dev), f32),
            pltpu.VMEM((rows, LANES), f32),
            pltpu.VMEM((n, own_rows, width), bf16),
            pltpu.VMEM((ntp * n - 1, own_rows, width), bf16),
            pltpu.VMEM((own_seqs, inner, LANES), f32),
            pltpu.VMEM((ntp, inner, own_seqs * LANES), bf16),
            pltpu.VMEM((ntp, 2, own_rows, LANES), f32),
            pltpu.VMEM((2 * head_size, state_len), bf16),
            pltpu.VMEM((LANES, LANES), bf16),
            pltpu.VMEM((7, own_rows * blocks, LANES), f32),
            pltpu.VMEM((own_rows * blocks, LANES), f32),
            pltpu.VMEM((n, own_rows, ntp * inner), bf16),
            pltpu.VMEM((3, own_rows * blocks, LANES), f32),
            pltpu.VMEM((3, own_rows * heads, LANES), f32),
            pltpu.VMEM((own_rows * heads, state_len), f32),
            dma((13,)),
            pltpu.SemaphoreType.REGULAR((1,)),
            dma((7,)),
            dma((6,)),
        ],
        compiler_params=pltpu.CompilerParams(
            collective_id=0, has_side_effects=True, vmem_limit_bytes=VMEM_LIMIT
        ),
    )(*map(hbm, (
        tokens, input_norm_gain.reshape(1, feature_dev), query_projection, key_projection,
        value_projection, write_strength_weight.T, decay_projection.T,
        head_decay_rate.reshape(1, heads), token_extra_decay, accepted, prior_step_states,
        output_norm_gain.reshape(1, head_size), output_projection,
    )))
    return pl.pallas_call(
        finish,
        out_shape=(
            jax.ShapeDtypeStruct(mixed.shape, bf16),
            jax.ShapeDtypeStruct(states.shape, f32),
        ),
        in_specs=[vmem_spec, vmem_spec],
        out_specs=(any_spec, any_spec),
        scratch_shapes=[dma((1 + own_rows,))],
        compiler_params=pltpu.CompilerParams(vmem_limit_bytes=VMEM_LIMIT // 4),
    )(mixed, states)


def solution(mesh):
    in_specs = (
        P("dp", None, "kv"),
        P("kv"),
        P("kv", "tp"),
        P("kv", "tp"),
        P("kv", "tp"),
        P("kv", "tp"),
        P("kv", "tp"),
        P("tp"),
        P(("dp", "kv"), None, "tp"),
        P(("dp", "kv")),
        P(("dp", "kv"), None, "tp", None),
        P(),
        P("tp", "kv"),
    )
    out_specs = (P("dp", None, "kv"), P(("dp", "kv"), None, "tp", None))
    body = functools.partial(per_device, mesh.shape["kv"], mesh.shape["tp"])
    return jax.shard_map(
        body, mesh=mesh, in_specs=in_specs, out_specs=out_specs, check_vma=False
    )
```
